512 devices in a mesh: sp: 32 (over z, core), tp: 16 (over y, x).
Axes of the slice: x: 4, y: 4, z: 16, core: 2. Of those that a mesh axis runs over, the one named last changes fastest.
Arguments:
- receptance: bfloat16 [8192, 4096], P('sp', 'tp'), may hold values from -6 to 6
- key_vectors: bfloat16 [8192, 4096], P('sp', 'tp'), may hold values from -13 to 13
- value_vectors: bfloat16 [8192, 4096], P('sp', 'tp'), may hold values from -6 to 6
- decay_logits: bfloat16 [8192, 4096], P('sp', 'tp'), may hold values from -20 to 2
- rate_logits: bfloat16 [8192, 4096], P('sp', 'tp'), may hold values from -8 to 4
- gate_logits: bfloat16 [8192, 4096], P('sp', 'tp'), may hold values from -6 to 6
- group_gain: float32 [4096], P('tp'), may hold values from 0.1 to 1.9
- residual: bfloat16 [8192, 4096], P('sp', 'tp'), may hold values from -24 to 24
- mixer_out: bfloat16 [4096, 4096], P(None, 'tp'), may hold values from -0.09375 to 0.09375
- norm_gain: float32 [4096], P('tp'), may hold values from 0.1 to 1.9
- expert_ids: int32 [8192, 2], P('sp'), may hold values from 0 to 31, as said below
- route_weight: float32 [8192, 2], P('sp'), may hold values from 0.25 to 1
- expert_gate: bfloat16 [32, 4096, 1024], P('sp', 'tp'), may hold values from -0.09375 to 0.09375
- expert_up: bfloat16 [32, 4096, 1024], P('sp', 'tp'), may hold values from -0.09375 to 0.09375
- expert_down: bfloat16 [32, 1024, 4096], P('sp', None, 'tp'), may hold values from -0.1875 to 0.1875
Outputs:
- updated: bfloat16 [8192, 4096], P('sp', 'tp')
The draws below stay inside these ranges and needn't reach their ends.
Inputs may be any that keep to these rules, and one draw needn't show every extreme that they name: `expert_ids`: the experts of a row are different and lie in one group of 8 consecutive experts. In the rows of one index of sp (aligned blocks of 256 rows) no expert is named by more than 32 rows, and in every such block some expert is named by exactly 32 rows.
All inputs are finite; a program needn't handle non-finite values.
Results may differ from the reference program's by a relative error of at most 0.013.
Values may be sent and summed in bfloat16 or wider, within the bound.
No kernel may reach another device: no remote copies, remote signals or barrier semaphores. Data moves between devices by JAX's collectives and lax.ppermute only.
A program may use at most 64 MiB of HBM per device.

```python
import math
import jax
import jax.numpy as jnp
from jax import lax

D = 4096
WIDTH = 4096
HEAD = 64
HEADS = 64
FF = 1024
GROUPS = 4
TOP = 2
TOK_SP = 256
EXPERTS = 32
GROUP_EXPERTS = 8
CAP = 32
SLOTS = 1024
TOKENS = 8192
CUTS = 16
DBLK = 256
N_SP = 32


def fast_heads(key, count):
    order = jax.random.permutation(jax.random.fold_in(key, 7101), HEADS)
    return order < count


def draw_decay_logits(key, part):
    flags = fast_heads(key, HEADS // 2)
    noise = 0.6 * jnp.clip(jax.random.normal(jax.random.fold_in(key, 2), (TOKENS, WIDTH), jnp.float32), -3.0, 3.0)
    per_head = jnp.where(flags, math.log(1.0 / 16.0), math.log(0.8 / TOKENS))
    base = jnp.repeat(per_head, HEAD)
    channel = 0.3 * jnp.clip(jax.random.normal(jax.random.fold_in(key, 3), (WIDTH,), jnp.float32), -3.0, 3.0)
    halves = TOKENS // (TOK_SP // 2)
    drift = jax.random.uniform(jax.random.fold_in(key, 4), (halves, 1), jnp.float32, -1.1, 1.1)
    drift = jnp.repeat(drift, TOK_SP // 2, axis=0)
    log_rate = jnp.minimum(base[None, :] + channel[None, :] + drift + noise, -0.7)
    shifted = log_rate + 0.5
    return (shifted - jnp.log1p(-jnp.exp(shifted))).astype(jnp.bfloat16)


def draw_rate_logits(key, part):
    flags = fast_heads(key, HEADS // 2)
    spread = 0.7 * jnp.clip(jax.random.normal(jax.random.fold_in(key, 5), (TOKENS, WIDTH), jnp.float32), -2.4, 2.4)
    mixed_channels = jax.random.bernoulli(jax.random.fold_in(key, 6), 0.5, (WIDTH,))
    strong = jnp.logical_or(jnp.repeat(flags, HEAD), mixed_channels)
    centre = jnp.where(strong, 2.3, -6.0)
    width_scale = jnp.where(strong, 1.0, 0.5)
    return (centre[None, :] + width_scale[None, :] * spread).astype(jnp.bfloat16)


def draw_key_vectors(key, part):
    direction = jnp.clip(jax.random.normal(jax.random.fold_in(key, 21), (HEADS, HEAD), jnp.float32), -3.0, 3.0)
    along = 1.0 + 0.4 * jnp.clip(jax.random.normal(jax.random.fold_in(key, 22), (TOKENS, HEADS), jnp.float32), -2.0, 2.0)
    rough = jnp.clip(jax.random.normal(jax.random.fold_in(key, 23), (TOKENS, HEADS, HEAD), jnp.float32), -4.0, 4.0)
    keys = 1.5 * along[:, :, None] * direction[None, :, :] + rough
    return keys.reshape(TOKENS, WIDTH).astype(jnp.bfloat16)


def draw_residual(key, part):
    column_blocks = max(D // 128, 1)
    scales = jnp.exp(jax.random.uniform(jax.random.fold_in(key, 11), (column_blocks,), jnp.float32, math.log(0.4), math.log(2.5)))
    scales = jnp.repeat(scales, D // column_blocks)
    base = jnp.clip(jax.random.normal(jax.random.fold_in(key, 12), (TOKENS, D), jnp.float32), -5.0, 5.0)
    return (base * scales[None, :]).astype(jnp.bfloat16)


def draw_expert_ids(key, part):
    anchor = jax.random.fold_in(key, 9001)
    full_group = jax.random.randint(jax.random.fold_in(anchor, 1), (), 0, GROUPS)
    full_lead = jax.random.randint(jax.random.fold_in(anchor, 2), (), 0, GROUP_EXPERTS)
    block_keys = jax.random.split(jax.random.fold_in(anchor, 3), TOKENS // TOK_SP)
    spots = jnp.arange(GROUPS, dtype=jnp.int32)
    others_width = max(GROUP_EXPERTS - 1, 1)

    def one_block(block_key):
        keys_here = jax.random.split(block_key, 5)
        order = jax.random.permutation(keys_here[0], TOK_SP).astype(jnp.int32)
        held = jax.random.randint(keys_here[1], (), CAP, TOK_SP // 2 + 1)
        shift = jax.random.randint(keys_here[2], (), 0, GROUPS - 1)
        leads = jax.random.randint(keys_here[3], (GROUPS,), 0, GROUP_EXPERTS)
        leads = jnp.where(spots == full_group, full_lead, leads)
        shuffles = jax.vmap(lambda subkey: jax.random.permutation(subkey, others_width))(jax.random.split(keys_here[4], GROUPS)).astype(jnp.int32)
        in_full = order < held
        others = order - held
        group = jnp.where(in_full, full_group, (full_group + 1 + (others + shift) % (GROUPS - 1)) % GROUPS)
        rank = jnp.where(in_full, order, others // (GROUPS - 1))
        lead = leads[group]
        shuffle_rows = shuffles[group]

        def other_expert(position):
            pick = jnp.take_along_axis(shuffle_rows, (position % others_width)[:, None], axis=1)[:, 0]
            return (lead + 1 + pick) % GROUP_EXPERTS
        early = rank < CAP
        late_pos = CAP + 2 * (rank - CAP)
        first_pick = jnp.where(early, lead, other_expert(late_pos))
        second_pick = jnp.where(early, other_expert(rank), other_expert(late_pos + 1))
        return jnp.stack([group * GROUP_EXPERTS + first_pick, group * GROUP_EXPERTS + second_pick], axis=1)
    chosen = jax.vmap(one_block)(block_keys)
    return chosen.reshape(TOKENS, TOP).astype(jnp.int32)


def block_levels(own_key, extent, pieces, least, top_value):
    def one(dim, parts):
        steps = jax.random.uniform(jax.random.fold_in(jax.random.fold_in(own_key, 6), dim), (parts,), jnp.float32, least / len(pieces), top_value / len(pieces))
        return jnp.repeat(jnp.exp(steps), extent[dim] // parts).reshape((-1,) + (1,) * (len(extent) - dim - 1))

    loudness = one(*pieces[0])
    for cut in pieces[1:]:
        loudness = loudness * one(*cut)
    return loudness


def normal_values(key, dims, width, bound, cuts=(), kind=jnp.bfloat16):
    values = jax.random.normal(key, dims, jnp.float32) * width
    if len(cuts) > 0:
        values = block_levels(key, dims, cuts, -0.22, 0.18) * values
    return jnp.clip(values, min=-bound, max=bound).astype(kind)


def setup_inputs(seed: int = 0) -> dict:
    key_list = jax.random.split(jax.random.key(seed), 16)
    return {
        "receptance": normal_values(key_list[0], (TOKENS, WIDTH), 1.0, 6.0, ((0, 32), (1, 16))),
        "key_vectors": draw_key_vectors(jax.random.fold_in(key_list[15], 71), 0),
        "value_vectors": normal_values(key_list[2], (TOKENS, WIDTH), 1.0, 6.0, ((0, 32), (1, 16))),
        "decay_logits": draw_decay_logits(jax.random.fold_in(key_list[15], 71), 0),
        "rate_logits": draw_rate_logits(jax.random.fold_in(key_list[15], 71), 0),
        "gate_logits": normal_values(key_list[5], (TOKENS, WIDTH), 1.5, 6.0, ((0, 32), (1, 16))),
        "group_gain": jnp.clip(1.0 + 0.18 * jax.random.normal(key_list[6], (WIDTH,), jnp.float32), 0.1, 1.9),
        "residual": draw_residual(jax.random.fold_in(key_list[15], 71), 0),
        "mixer_out": normal_values(key_list[8], (WIDTH, D), WIDTH ** -0.5, 0.09375, ((1, 16),)),
        "norm_gain": jnp.clip(1.0 + 0.18 * jax.random.normal(key_list[9], (D,), jnp.float32), 0.1, 1.9),
        "expert_ids": draw_expert_ids(jax.random.fold_in(key_list[15], 71), 0),
        "route_weight": jnp.clip(0.25 + 0.75 * jax.random.uniform(key_list[11], (TOKENS, TOP), jnp.float32) ** block_levels(key_list[11], (TOKENS, TOP), ((0, 32),), -0.2, 0.2), 0.25, 1.0),
        "expert_gate": normal_values(key_list[12], (EXPERTS, D, FF), D ** -0.5, 0.09375, ((0, 32), (1, 16))),
        "expert_up": normal_values(key_list[13], (EXPERTS, D, FF), D ** -0.5, 0.09375, ((0, 32), (1, 16))),
        "expert_down": normal_values(key_list[14], (EXPERTS, FF, D), FF ** -0.5, 0.1875, ((0, 32), (2, 16))),
    }


EPS_GROUP = 0.00064
EPS_NORM = 1e-06
HIGHEST = lax.Precision.HIGHEST

def by_heads(array):
    return array.astype(jnp.float32).reshape(array.shape[0], WIDTH // HEAD, HEAD)

def time_mix(receptance, key_vectors, value_vectors, decay_logits, rate_logits, gate_logits, group_gain):
    recept = by_heads(receptance)
    keyvec = by_heads(key_vectors)
    valvec = by_heads(value_vectors)
    decay = jnp.exp(-jnp.exp(-jax.nn.softplus(-by_heads(decay_logits)) - 0.5))
    unit_key = keyvec / jnp.sqrt(1.0 + lax.optimization_barrier(jnp.sum(keyvec * keyvec, axis=-1, keepdims=True)))
    correction = unit_key * jax.nn.sigmoid(by_heads(rate_logits))

    def advance(carried, inputs):
        recept_now, decay_now, key_now, value_now, unit_now, corr_now = inputs
        pulled = jnp.einsum('hij,hj->hi', carried, unit_now, precision=HIGHEST)
        carried = carried * decay_now[:, None, :] - pulled[:, :, None] * corr_now[:, None, :] + value_now[:, :, None] * key_now[:, None, :]
        return (carried, jnp.einsum('hij,hj->hi', carried, recept_now, precision=HIGHEST))
    initial = jnp.zeros((WIDTH // HEAD, HEAD, HEAD), jnp.float32)
    final_state, state_read = lax.scan(advance, initial, (recept, decay, keyvec, valvec, unit_key, correction))
    centred = state_read - lax.optimization_barrier(jnp.mean(state_read, axis=-1, keepdims=True))
    scaled = centred * lax.rsqrt(lax.optimization_barrier(jnp.mean(centred * centred, axis=-1, keepdims=True)) + EPS_GROUP)
    gated_out = scaled.reshape(TOKENS, WIDTH) * group_gain.astype(jnp.float32)[None, :] * jax.nn.sigmoid(gate_logits.astype(jnp.float32))
    return gated_out.astype(jnp.bfloat16)

def block_ranks(expert_ids):
    grouped = expert_ids.reshape(N_SP, TOK_SP * TOP)
    onehot = (grouped[:, :, None] == jnp.arange(EXPERTS, dtype=jnp.int32)[None, None, :]).astype(jnp.int32)
    earlier = jnp.cumsum(onehot, axis=1) - onehot
    return lax.optimization_barrier(jnp.sum(earlier * onehot, axis=2)).reshape(TOKENS, TOP).astype(jnp.int32)

def cut_product(chosen, matrix):
    rows_cut = chosen.astype(jnp.float32).reshape(chosen.shape[0], CUTS, DBLK)
    matrix_cut = matrix.astype(jnp.float32).reshape(CUTS, DBLK, matrix.shape[1])
    partials = jnp.einsum('scd,cdf->csf', rows_cut, matrix_cut)
    rounded = lax.optimization_barrier(partials.astype(jnp.bfloat16))
    return lax.optimization_barrier(jnp.sum(rounded.astype(jnp.float32), axis=0))

def reference(receptance, key_vectors, value_vectors, decay_logits, rate_logits, gate_logits, group_gain, residual, mixer_out, norm_gain, expert_ids, route_weight, expert_gate, expert_up, expert_down):
    mixed_rows = time_mix(receptance, key_vectors, value_vectors, decay_logits, rate_logits, gate_logits, group_gain)
    midway = (residual.astype(jnp.float32) + jnp.dot(mixed_rows, mixer_out, preferred_element_type=jnp.float32)).astype(jnp.bfloat16)
    midway_f = midway.astype(jnp.float32)
    inv_rms = lax.rsqrt(lax.optimization_barrier(jnp.mean(midway_f * midway_f, axis=1, keepdims=True)) + EPS_NORM)
    normed = (midway_f * norm_gain.astype(jnp.float32)[None, :] * inv_rms).astype(jnp.bfloat16)
    ranks = block_ranks(expert_ids)
    token_ids = jnp.arange(TOKENS, dtype=jnp.int32)
    within = ((token_ids // TOK_SP)[:, None] * CAP + ranks).astype(jnp.int32)
    owners = jnp.broadcast_to(token_ids[:, None], expert_ids.shape).astype(jnp.int32)
    slot_table = jnp.full((EXPERTS, SLOTS), TOKENS, jnp.int32).at[expert_ids, within].set(owners)
    slot_weight = jnp.zeros((EXPERTS, SLOTS), jnp.float32).at[expert_ids, within].set(route_weight.astype(jnp.float32))
    padded = jnp.concatenate([normed, jnp.zeros((1, D), jnp.bfloat16)], axis=0)

    def one_expert(running, inputs):
        table_row, weight_row, gate_mat, up_mat, down_mat = inputs
        chosen = padded[table_row]
        hidden = (jax.nn.silu(cut_product(chosen, gate_mat)) * cut_product(chosen, up_mat)).astype(jnp.bfloat16)
        result = jnp.dot(hidden, down_mat, preferred_element_type=jnp.float32).astype(jnp.bfloat16)
        running = running.at[table_row].add(result.astype(jnp.float32) * weight_row[:, None])
        return (running, None)
    routed, unused = lax.scan(one_expert, jnp.zeros((TOKENS + 1, D), jnp.float32), (slot_table, slot_weight, expert_gate, expert_up, expert_down))
    return (midway_f + routed[:TOKENS]).astype(jnp.bfloat16)
```

```python
import jax
import jax.numpy as jnp
from jax import lax
from jax.experimental import pallas as pl
from jax.experimental.pallas import tpu as pltpu
from jax.sharding import Mesh
from jax.sharding import PartitionSpec as P

D = 4096
SP = ("sp_0", "sp_1")
EPS_NORM = 1e-06
HEAD = 64
SPAN = 64
SUB = 16
LANES = 128
NT = (((1,), (1,)), ((), ()))
NN = (((1,), (0,)), ((), ()))
TN = (((0,), (0,)), ((), ()))
EPS_GROUP = 0.00064
F32 = jnp.float32
BF16 = jnp.bfloat16


def dot(a, b, dims):
    return lax.dot_general(a, b, dims, preferred_element_type=F32)


def split(a):
    high = a.astype(BF16)
    return high, (a - high.astype(F32)).astype(BF16)


def dot_exact(a, b, dims):
    a_high, a_low = split(a)
    b_high, b_low = split(b)
    return dot(a_high, b_high, dims) + (dot(a_high, b_low, dims) + dot(a_low, b_high, dims))


def dot_left(a, b, dims):
    a_high, a_low = split(a)
    return dot(a_high, b, dims) + dot(a_low, b, dims)


def dot_right(a, b, dims):
    b_high, b_low = split(b)
    return dot(a, b_high, dims) + dot(a, b_low, dims)


def iota(shape, dim):
    return lax.broadcasted_iota(jnp.int32, shape, dim)


def head_sums(values):
    width = values.shape[1]
    ones = (iota((width, width), 0) // HEAD == iota((width, width), 1) // HEAD).astype(F32).astype(BF16)
    return dot_left(values, ones, NN)


def paired_diag(pair):
    first = iota(pair.shape, 1) < HEAD
    return jnp.concatenate([jnp.where(first, pair, 0.0), jnp.where(first, 0.0, pair)], axis=0)


def follow(earlier, later):
    carried = dot_exact(earlier, paired_diag(later[HEAD:]), NN)
    return jnp.concatenate([carried[:HEAD] + later[:HEAD], carried[HEAD:]], axis=0)


def state_kernel(r_ref, k_ref, v_ref, d_ref, b_ref, local_ref, start_ref, prefix_ref, total_ref, low_ref, x_ref):
    tokens, width = k_ref.shape
    heads = width // HEAD
    spans = tokens // SPAN
    pairs = heads // 2
    key = k_ref[...].astype(F32)
    recept = r_ref[...].astype(F32)
    unit = key * lax.rsqrt(1.0 + head_sums(key * key))
    corr = unit * jax.nn.sigmoid(b_ref[...].astype(F32))
    logdec = -0.6065306597126334 * jax.nn.sigmoid(d_ref[...].astype(F32))
    lower = (iota((SPAN, SPAN), 1) <= iota((SPAN, SPAN), 0)).astype(F32).astype(BF16)
    lane_head = iota((SPAN, width), 1) // HEAD
    tall = heads * SPAN
    place = iota((tall, LANES), 0) % SPAN
    source = iota((tall, LANES), 1) % SPAN
    first = iota((SPAN, LANES), 1) < HEAD
    reads = []
    kept = []
    for n in range(spans):
        rows = slice(n * SPAN, (n + 1) * SPAN)
        ld = logdec[rows]
        ld_high, ld_rest = split(ld)
        ld_low = (ld - ld_high.astype(F32) - ld_rest.astype(F32)).astype(BF16)
        cum = dot(lower, ld_high, NN) + (dot(lower, ld_rest, NN) + dot(lower, ld_low, NN))
        end = cum[SPAN - 1 :]
        grow = jnp.exp(-cum)
        tail = jnp.exp(end - cum)
        r_in = recept[rows] * jnp.exp(cum)
        u_in = unit[rows] * jnp.exp(cum - ld)
        k_out = key[rows] * grow
        c_out = corr[rows] * grow
        k_tail = key[rows] * tail
        c_tail = corr[rows] * tail
        queries = jnp.concatenate(
            [jnp.where(lane_head == h, q, 0.0) for q in (u_in, r_in) for h in range(heads)], axis=0
        )
        pulls = dot_exact(queries, jnp.concatenate([c_out, k_out], axis=0), NT)
        pull_u = jnp.where(source < place, pulls[:tall], 0.0)
        pull_r = jnp.where(source <= place, pulls[tall:], 0.0)
        value = v_ref[rows, :]
        both = jnp.concatenate([pull_u, pull_r], axis=0)[:, HEAD:]
        by_value = dot_left(both, value, NN)
        low_ref[pl.ds(n * tall, tall), :] = pull_u
        for h in range(heads):
            p = h // 2
            lanes = slice(p * LANES, (p + 1) * LANES)
            kv = by_value[h * SPAN : (h + 1) * SPAN, lanes]
            krv = by_value[tall + h * SPAN : tall + (h + 1) * SPAN, lanes]
            u_tile = u_in[:, lanes]
            r_tile = r_in[:, lanes]
            if h % 2 == 0:
                rhs = jnp.where(first, kv, pltpu.roll(u_tile, HEAD, 1))
                base = jnp.where(first, krv, pltpu.roll(r_tile, HEAD, 1))
            else:
                rhs = jnp.where(first, pltpu.roll(kv, HEAD, 1), u_tile)
                base = jnp.where(first, pltpu.roll(krv, HEAD, 1), r_tile)
            x_ref[pl.ds((n * heads + h) * SPAN, SPAN), :] = rhs
            reads.append((base, pull_r[h * SPAN : (h + 1) * SPAN, :HEAD]))
        kept.append((c_tail, k_tail, end))
    systems = spans * heads
    for b in range(SPAN // SUB):
        if b > 0:
            for s in range(systems):
                at = s * SPAN
                done = x_ref[at : at + b * SUB, :]
                coef = low_ref[at + b * SUB : at + (b + 1) * SUB, : b * SUB]
                x_ref[at + b * SUB : at + (b + 1) * SUB, :] = x_ref[
                    at + b * SUB : at + (b + 1) * SUB, :
                ] - dot_exact(coef, done, NN)
        solved = []
        for t in range(b * SUB, (b + 1) * SUB):
            now = x_ref[pl.ds(t, systems, stride=SPAN), :]
            coef = low_ref[pl.ds(t, systems, stride=SPAN), :]
            for s in range(b * SUB, t):
                now = now - coef[:, s : s + 1] * solved[s - b * SUB]
            solved.append(now)
            x_ref[pl.ds(t, systems, stride=SPAN), :] = now
    prefix = [None] * pairs
    for n in range(spans):
        rows = slice(n * SPAN, (n + 1) * SPAN)
        c_tail, k_tail, end = kept[n]
        for p in range(pairs):
            lanes = slice(p * LANES, (p + 1) * LANES)
            value = v_ref[rows, lanes].astype(F32)
            stacked = jnp.concatenate([c_tail[:, lanes], k_tail[:, lanes]], axis=0)
            out = []
            steps = []
            for q in range(2):
                h = 2 * p + q
                x = x_ref[(n * heads + h) * SPAN : (n * heads + h + 1) * SPAN, :]
                base, coef = reads[n * heads + h]
                out.append(base - dot_exact(coef, x, NN))
                own = jnp.where(first, value if q == 0 else pltpu.roll(value, HEAD, 1), 0.0)
                steps.append(dot_exact(jnp.concatenate([-x, own], axis=0), stacked, TN))
            local_ref[rows, lanes] = jnp.where(first, out[0], pltpu.roll(out[1], HEAD, 1))
            start_ref[rows, lanes] = jnp.where(first, pltpu.roll(out[0], HEAD, 1), out[1])
            wide = iota((2 * HEAD, LANES), 1)
            step = jnp.where(wide < HEAD, steps[0], steps[1])
            keep = jnp.exp(end[:, lanes])
            step = step + jnp.where(wide % HEAD + HEAD == iota((2 * HEAD, LANES), 0), keep, 0.0)
            prefix[p] = step if n == 0 else follow(prefix[p], step)
            if n < spans - 1:
                prefix_ref[p, n] = prefix[p]
            else:
                total_ref[p] = prefix[p].astype(total_ref.dtype)


def state_pieces(r, k, v, d, b):
    tokens, width = k.shape
    heads, spans = width // HEAD, tokens // SPAN
    pairs = heads // 2
    return pl.pallas_call(
        state_kernel,
        out_shape=(
            jax.ShapeDtypeStruct((tokens, width), F32),
            jax.ShapeDtypeStruct((tokens, width), F32),
            jax.ShapeDtypeStruct((pairs, spans - 1, 2 * HEAD, LANES), F32),
            jax.ShapeDtypeStruct((pairs, 2 * HEAD, LANES), BF16),
        ),
        scratch_shapes=[
            pltpu.VMEM((heads * tokens, LANES), F32),
            pltpu.VMEM((heads * tokens, LANES), F32),
        ],
    )(r, k, v, d, b)


def read_kernel(local_ref, start_ref, prefix_ref, in_ref, g_ref, gain_ref, out_ref):
    tokens, width = local_ref.shape
    spans = tokens // SPAN
    for n in range(spans):
        rows = slice(n * SPAN, (n + 1) * SPAN)
        tiles = []
        for p in range(width // LANES):
            lanes = slice(p * LANES, (p + 1) * LANES)
            state = in_ref[p].astype(F32)
            if n > 0:
                before = prefix_ref[p, n - 1]
                state = dot_exact(state, paired_diag(before[HEAD:]), NN) + before[:HEAD]
            tiles.append(local_ref[rows, lanes] + dot_exact(start_ref[rows, lanes], paired_diag(state), NT))
        read = jnp.concatenate(tiles, axis=1)
        centred = read - head_sums(read) * (1.0 / HEAD)
        spread = head_sums(centred * centred) * (1.0 / HEAD)
        scaled = centred * lax.rsqrt(spread + EPS_GROUP)
        gate = jax.nn.sigmoid(g_ref[rows, :].astype(F32))
        out_ref[rows, :] = (scaled * gain_ref[...] * gate).astype(out_ref.dtype)


def mixed_rows(local, start, prefix, incoming, gate_logits, gain):
    return pl.pallas_call(
        read_kernel,
        out_shape=jax.ShapeDtypeStruct(local.shape, BF16),
    )(local, start, prefix, incoming, gate_logits, gain)


def carried_in(shard, axes):
    before, so_far = None, shard
    for axis in reversed(axes):
        size, mine = lax.axis_size(axis), lax.axis_index(axis)
        pieces = lax.all_gather(so_far.astype(BF16), axis)
        inside, total = combine(pieces, mine)
        before = inside if before is None else join(inside, before)
        so_far = total
    return before[:, :HEAD]


def combine_kernel(mine_ref, pieces_ref, inside_ref, total_ref):
    size, pairs = pieces_ref.shape[0], pieces_ref.shape[1]
    mine = mine_ref[0]
    for p in range(pairs):
        so_far = pieces_ref[0, p].astype(F32)
        first = iota((2 * HEAD, LANES), 1) % HEAD + HEAD == iota((2 * HEAD, LANES), 0)
        inside = jnp.where(mine > 0, so_far, first.astype(F32))
        for n in range(1, size):
            so_far = follow(so_far, pieces_ref[n, p].astype(F32))
            inside = jnp.where(mine > n, so_far, inside)
        inside_ref[p] = inside
        total_ref[p] = so_far


def combine(pieces, mine):
    shape = jax.ShapeDtypeStruct(pieces.shape[1:], F32)
    return pl.pallas_call(
        combine_kernel,
        in_specs=[pl.BlockSpec(memory_space=pltpu.SMEM), pl.BlockSpec(memory_space=pltpu.VMEM)],
        out_shape=(shape, shape),
    )(mine.reshape(1).astype(jnp.int32), pieces)


def join_kernel(earlier_ref, later_ref, out_ref):
    for p in range(out_ref.shape[0]):
        out_ref[p] = follow(earlier_ref[p], later_ref[p])


def join(earlier, later):
    return pl.pallas_call(join_kernel, out_shape=jax.ShapeDtypeStruct(later.shape, F32))(earlier, later)


def time_mix(receptance, key_vectors, value_vectors, decay_logits, rate_logits, gate_logits, group_gain):
    read_local, start_rows, prefix, total = state_pieces(
        receptance, key_vectors, value_vectors, decay_logits, rate_logits
    )
    incoming = carried_in(total, SP)
    return mixed_rows(read_local, start_rows, prefix, incoming, gate_logits, group_gain[None, :])


def from_everyone(shard, axis):
    size = lax.axis_size(axis)
    return lax.all_to_all(
        jnp.broadcast_to(shard[None], (size, *shard.shape)), axis, 0, 0, tiled=True
    )


def joined_along(pieces, dim):
    dims = list(pieces.shape[1:])
    dims[dim] *= pieces.shape[0]
    return jnp.moveaxis(pieces, 0, dim).reshape(dims)


def gather_directly(shard, axis, dim):
    pieces = from_everyone(shard, axis)
    return joined_along(pieces, dim)


def of_everyone(shard, axis):
    everything = from_everyone(shard, axis)
    return jnp.sum(everything, axis=0)


def split_up(shard, dim, size):
    before, after = (shard.shape[:dim], shard.shape[dim + 1 :])
    return jnp.moveaxis(shard.reshape(*before, size, -1, *after), dim, 0)


def sent_and_summed(shard, axis, dim):
    size = lax.axis_size(axis)
    pieces = lax.all_to_all(split_up(shard, dim, size), axis, 0, 0, tiled=True)
    return jnp.sum(pieces.astype(jnp.float32), axis=0)


def local(
    receptance,
    key_vectors,
    value_vectors,
    decay_logits,
    rate_logits,
    gate_logits,
    group_gain,
    residual,
    mixer_out,
    norm_gain,
    expert_ids,
    route_weight,
    expert_gate,
    expert_up,
    expert_down,
):
    mixed_rows = time_mix(
        receptance, key_vectors, value_vectors, decay_logits, rate_logits, gate_logits, group_gain
    )
    tokens_here, features = residual.shape
    projected = jnp.dot(
        gather_directly(mixed_rows, "tp", 1), mixer_out, preferred_element_type=jnp.float32
    )
    midway = (residual.astype(jnp.float32) + projected).astype(jnp.bfloat16)
    midway_f = midway.astype(jnp.float32)
    squares = of_everyone(jnp.sum(midway_f * midway_f, axis=1), "tp")
    inv_rms = lax.rsqrt(squares / D + EPS_NORM)
    normed = (midway_f * norm_gain[None, :] * inv_rms[:, None]).astype(jnp.bfloat16)
    routes = expert_ids.shape[1]
    experts_all = lax.axis_size(SP) * expert_gate.shape[0]
    capacity = 2 * tokens_here * routes // experts_all
    flat_ids = expert_ids.reshape(-1)
    onehot = (flat_ids[:, None] == jnp.arange(experts_all, dtype=jnp.int32)[None, :]).astype(
        jnp.int32
    )
    earlier_count = jnp.sum((jnp.cumsum(onehot, axis=0) - onehot) * onehot, axis=1)
    slot_of = flat_ids * capacity + earlier_count
    owner_token = jnp.arange(tokens_here * routes, dtype=jnp.int32) // routes
    slot_table = (
        jnp.full((experts_all * capacity,), tokens_here, jnp.int32).at[slot_of].set(owner_token)
    )
    padded = jnp.concatenate([normed, jnp.zeros((1, features), jnp.bfloat16)], axis=0)
    outgoing = padded[slot_table].reshape(experts_all, capacity, features)
    arrived = lax.all_to_all(outgoing, SP, split_axis=0, concat_axis=0, tiled=True)
    arrived_rows = arrived.reshape(-1, features)
    paired = jnp.concatenate([expert_gate[0], expert_up[0]], axis=1)
    gate_up = sent_and_summed(
        jnp.dot(arrived_rows, paired, preferred_element_type=jnp.float32).astype(jnp.bfloat16),
        "tp",
        0,
    )
    half_width = paired.shape[1] // 2
    hidden = (jax.nn.silu(gate_up[:, :half_width]) * gate_up[:, half_width:]).astype(jnp.bfloat16)
    expert_res = jnp.dot(
        gather_directly(hidden, "tp", 0), expert_down[0], preferred_element_type=jnp.float32
    )
    returned = lax.all_to_all(
        expert_res.astype(jnp.bfloat16).reshape(-1, capacity, features),
        SP,
        split_axis=0,
        concat_axis=0,
        tiled=True,
    )
    picked = (
        returned.reshape(-1, features)[slot_of]
        .astype(jnp.float32)
        .reshape(tokens_here, routes, features)
    )
    routed_sum = jnp.sum(picked * route_weight[:, :, None], axis=1)
    return (midway_f + routed_sum).astype(jnp.bfloat16)


def solution(mesh):
    torus = Mesh(mesh.devices.reshape(16, 2, mesh.shape["tp"]), ("sp_0", "sp_1", "tp"))
    return jax.shard_map(
        local,
        mesh=torus,
        in_specs=(
            P(SP, "tp"),
            P(SP, "tp"),
            P(SP, "tp"),
            P(SP, "tp"),
            P(SP, "tp"),
            P(SP, "tp"),
            P("tp"),
            P(SP, "tp"),
            P(None, "tp"),
            P("tp"),
            P(SP, None),
            P(SP, None),
            P(SP, "tp", None),
            P(SP, "tp", None),
            P(SP, None, "tp"),
        ),
        out_specs=P(SP, "tp"),
        check_vma=False,
    )
```
